512 devices in a mesh: ep: 32 (over z, core), tp: 16 (over y, x).
Axes of the slice: x: 4, y: 4, z: 16, core: 2. Of those that a mesh axis runs over, the one named last changes fastest.
Arguments:
- tokens: bfloat16 [1024, 2048], P('ep', 'tp'), may hold values from -200 to 200
- routing: int32 [1024, 4], P('ep'), may hold values from 0 to 63, all different within a row; in each aligned block of 32 rows (0 to 31, 32 to 63, ...) at most 8 rows name the same one
- gate_weights: float32 [1024, 4], P('ep'), may hold values from 0.05 to 1
- norm_gain: float32 [2048], replicated, may hold values from 0.1 to 1.9
- w_gate: bfloat16 [64, 2048, 2048], P('ep', None, 'tp'), may hold values from -0.33007812 to 0.33007812
- w_up: bfloat16 [64, 2048, 2048], P('ep', None, 'tp'), may hold values from -0.33007812 to 0.33007812
- w_down: bfloat16 [64, 2048, 2048], P('ep', 'tp'), may hold values from -0.026489258 to 0.026489258
Outputs:
- mixed: bfloat16 [1024, 2048], P('ep', 'tp')
The draws below stay inside these ranges and needn't reach their ends.
Inputs may be any that keep to these rules, and one draw needn't show every extreme that they name: `routing`: each token names 4 different experts. Among the 32 tokens of one index of ep no expert is named more than 8 times, a bound that some block reaches.
All inputs are finite; a program needn't handle non-finite values.
Results may differ from the reference program's by a relative error of at most 0.015.
Values may be sent and summed in bfloat16 or wider, within the bound.
No kernel may reach another device: no remote copies, remote signals or barrier semaphores. Data moves between devices by JAX's collectives and lax.ppermute only.
A program may use at most 128 MiB of HBM per device.

```python
import math
import jax
import jax.numpy as jnp
import numpy as np
from jax import lax

D = 2048
FF = 2048
TOP = 4
EXP_DEV = 2
TOK_DEV = 32
CAP = 8
EXPERTS = 64
TOKENS = 1024
N_EP = 32
N_TP = 16


def draw_tokens(key, part):
    base_key, scale_key, row_key, mean_key = jax.random.split(key, 4)
    values = jax.random.normal(base_key, (TOKENS, D), jnp.float32)
    values = jnp.clip(values, -6.0, 6.0)
    column_scale = jnp.exp(jax.random.uniform(scale_key, (D // 16,), jnp.float32, jnp.log(0.3), jnp.log(3.0)))
    values = values * jnp.repeat(column_scale, 16)[None, :]
    return values.astype(jnp.bfloat16)


def block_levels(stream_key, dims, cuts, smallest, top_value):
    loudness = 1.0
    for axis_at, shards_of in cuts:
        draws = jax.random.uniform(jax.random.fold_in(jax.random.fold_in(stream_key, 6), axis_at), (shards_of,), jnp.float32, smallest / len(cuts), top_value / len(cuts))
        loudness = loudness * jnp.repeat(jnp.exp(draws), dims[axis_at] // shards_of).reshape((-1,) + (1,) * (len(dims) - 1 - axis_at))
    return loudness


def routed_block(key, own, number, rows, count, top, most, skew):
    order = jax.random.permutation(key, count)
    crowded, common = load_shares(count, rows * top, most, skew, True), load_shares(count, rows * top, most, skew, False)
    places = jnp.arange(count)

    def named(lengths, rotation):
        used = int((lengths > 0).sum())
        fixed = max(1, used // 4)
        moved = fixed + (places - fixed + rotation * (used - fixed)) % max(1, count - fixed)
        return jnp.zeros((count,), jnp.int32).at[order[jnp.where(places < fixed, places, moved)]].set(jnp.asarray(lengths, jnp.int32))

    lengths = jnp.where(number % 4 == 0, named(crowded, number // 4), named(common, number - number // 4 - 1))
    mixed = jax.random.permutation(jax.random.fold_in(own, 3), count)
    giver, taker = mixed[0:count // 2 * 2:2], mixed[1:count // 2 * 2:2]
    room = jnp.minimum(lengths[giver] - 1, most - lengths[taker]) // 2
    room = jnp.where((giver == order[0]) | (taker == order[0]) | (lengths[taker] == 0), 0, jnp.maximum(room, 0))
    moved = jax.random.randint(jax.random.fold_in(own, 4), (count // 2,), 0, 1 << 20) % (room + 1)
    lengths = lengths.at[giver].add(-moved).at[taker].add(moved)
    members = jnp.searchsorted(jnp.cumsum(lengths), jnp.arange(rows * top), side="right").astype(jnp.int32)
    listing = members.reshape(top, rows).T
    listing = listing[jax.random.permutation(jax.random.fold_in(own, 1), rows)]
    rotation = jax.random.randint(jax.random.fold_in(own, 2), (rows, 1), 0, top)
    return jnp.take_along_axis(listing, (jnp.arange(top)[None, :] + rotation) % top, axis=1)


def load_shares(amount, total, most, slope, full):
    weights = [(1 << 20) // math.isqrt(grade ** slope) + 1 for grade in range(1, amount + 1)]
    largest = most if full else min(most, max(-(-total // amount), total * weights[0] // sum(weights)))
    least = 1 if total - largest >= amount - 1 else 0
    counts, rest = [largest] + [least] * (amount - 1), total - largest - least * (amount - 1)
    while rest > 0:
        free = [i for i in range(1, amount) if counts[i] < largest] or [i for i in range(1, amount) if counts[i] < most]
        whole, left = sum([weights[i] for i in free]), rest
        for i in free:
            more = min(most - counts[i], max(1, left * weights[i] // whole), rest)
            counts[i] = counts[i] + more
            rest = rest - more
    return np.array(counts)


def scatter_about(key, shape, deviation, reach, pieces=(), held_as=jnp.bfloat16):
    drawn = deviation * jax.random.normal(key, shape, jnp.float32)
    if pieces:
        drawn = drawn * block_levels(key, shape, pieces, -0.22, 0.18)
    return jnp.clip(drawn, -reach, reach).astype(held_as)


def setup_inputs(seed: int = 0) -> dict:
    keys = jax.random.split(jax.random.key(seed), 8)
    tokens = draw_tokens(jax.random.fold_in(keys[7], 71), 0)
    routing_keys = jax.random.split(jax.random.fold_in(keys[1], 1), TOKENS // TOK_DEV)
    routing_turns = jax.random.permutation(jax.random.fold_in(keys[1], 3), TOKENS // TOK_DEV)
    routing = jax.vmap(lambda own, number: routed_block(jax.random.fold_in(keys[1], 2), own, number, TOK_DEV, EXP_DEV * N_EP, TOP, CAP, 2))(routing_keys, routing_turns).reshape((TOKENS, TOP))
    gate_weights = jnp.clip(jnp.exp(math.log(1.0) - 2.9957323 * jax.random.uniform(keys[2], (TOKENS, TOP), jnp.float32) ** block_levels(keys[2], (TOKENS, TOP), ((0, 32),), -0.2, 0.2)), 0.05, 1.0)
    norm_gain = jnp.clip(1.0 + 0.18 * jax.random.normal(keys[3], (D,), jnp.float32), 0.1, 1.9)
    w_gate = scatter_about(keys[4], (EXPERTS, D, FF), (2.5 * D ** -0.5), 0.33007812, ((0, 32), (2, 16)))
    w_up = scatter_about(keys[5], (EXPERTS, D, FF), (2.5 * D ** -0.5), 0.33007812, ((0, 32), (2, 16)))
    w_down = scatter_about(keys[6], (EXPERTS, FF, D), (0.2 * FF ** -0.5), 0.026489258, ((0, 32), (1, 16)))
    return dict(tokens=tokens, routing=routing, gate_weights=gate_weights, norm_gain=norm_gain, w_gate=w_gate, w_up=w_up, w_down=w_down)


norm_eps = 1e-06
clamp_limit = 7.0
swish_alpha = 1.702

def expert_apply(inputs):
    rows, gate_mat, up_mat, down_mat = inputs
    pre_gate = jnp.dot(rows, gate_mat, preferred_element_type=jnp.float32)
    pre_up = jnp.dot(rows, up_mat, preferred_element_type=jnp.float32)
    clamped = jnp.minimum(pre_gate, clamp_limit)
    upper = jnp.clip(pre_up, -clamp_limit, clamp_limit)
    hidden = (clamped * jax.nn.sigmoid(swish_alpha * clamped) * (upper + 1.0)).astype(jnp.bfloat16)
    block_width = FF // N_TP
    hidden_blocks = hidden.reshape(hidden.shape[0], N_TP, block_width).astype(jnp.float32)
    down_blocks = down_mat.reshape(N_TP, block_width, D).astype(jnp.float32)
    partial_value = jnp.einsum('rnf,nfd->nrd', hidden_blocks, down_blocks)
    rounded = partial_value.astype(jnp.bfloat16).astype(jnp.float32)
    return lax.optimization_barrier(jnp.sum(rounded, axis=0)).astype(jnp.bfloat16)

def reference(tokens, routing, gate_weights, norm_gain, w_gate, w_up, w_down):
    expert_count = EXP_DEV * N_EP
    wide = tokens.astype(jnp.float32)
    ssq = lax.optimization_barrier(jnp.sum(wide * wide, axis=1, keepdims=True))
    normed = (wide * lax.rsqrt(ssq / D + norm_eps) * norm_gain[None, :]).astype(jnp.bfloat16)
    grouped = routing.reshape(N_EP, TOK_DEV * TOP)
    onehot = (grouped[:, :, None] == jnp.arange(expert_count, dtype=jnp.int32)[None, None, :]).astype(jnp.int32)
    slot_rank = lax.optimization_barrier(jnp.sum(jnp.cumsum(onehot, axis=1) * onehot, axis=2)) - 1
    groups = jnp.arange(N_EP, dtype=jnp.int32)[:, None]
    slot_index = (grouped * (N_EP * CAP) + groups * CAP + slot_rank).reshape(-1).astype(jnp.int32)
    repeated = jnp.repeat(normed, TOP, axis=0)
    buffer = jnp.zeros((expert_count * N_EP * CAP, D), jnp.bfloat16).at[slot_index].set(repeated)
    buffer = buffer.reshape(expert_count, N_EP * CAP, D)
    expert_out = lax.map(expert_apply, (buffer, w_gate, w_up, w_down))
    picked = expert_out.reshape(-1, D)[slot_index].astype(jnp.float32).reshape(TOKENS, TOP, D)
    mixed = lax.optimization_barrier(jnp.sum(gate_weights[:, :, None] * picked, axis=1))
    return mixed.astype(jnp.bfloat16)
```

```python
import functools

import jax
import jax.numpy as jnp
from jax import lax
from jax.experimental import pallas as pl
from jax.experimental.pallas import tpu as pltpu
from jax.sharding import Mesh
from jax.sharding import PartitionSpec as P

D = 2048
CAP = 8
TP = ("tp_0", "tp_1")
BUCKETS = (512,)

norm_eps = 1e-06
clamp_limit = 7.0
swish_alpha = 1.702
EMPTY = 512.0
FILLED_BELOW = 256.0

f32 = jnp.float32
bf16 = jnp.bfloat16
VMEM = pl.BlockSpec(memory_space=pltpu.VMEM)
SMEM = pl.BlockSpec(memory_space=pltpu.SMEM)
ANY = pl.BlockSpec(memory_space=pl.ANY)


def iota(shape, dim):
    return lax.broadcasted_iota(jnp.int32, shape, dim)


def dot(a, b):
    return jnp.dot(a, b, preferred_element_type=f32)


def dispatch_kernel(routing_ref, weight_ref, tokens_ref, out_ref, high_ref, low_ref):
    slots = out_ref.shape[0]
    top, rows = routing_ref.shape
    slot = iota((slots, rows), 0)
    expert = slot // CAP
    chosen = jnp.zeros((slots, rows), f32)
    weight = jnp.zeros((slots, rows), f32)
    for k in range(top):
        match = routing_ref[k : k + 1, :] == expert
        chosen = jnp.where(match, 1.0, chosen)
        weight = jnp.where(match, weight_ref[k : k + 1, :], weight)
    before = (iota((rows, rows), 0) < iota((rows, rows), 1)).astype(f32).astype(bf16)
    rank = dot(chosen.astype(bf16), before).astype(jnp.int32)
    placed = jnp.where(rank == slot % CAP, chosen, 0.0)
    placing = placed.astype(bf16)
    rows_out = dot(placing, tokens_ref[...])
    filled = dot(placing, jnp.ones((rows, out_ref.shape[1]), bf16))
    out_ref[...] = jnp.where(filled > 0.5, rows_out, EMPTY).astype(bf16)
    weight = weight * placed
    high = weight.astype(bf16)
    high_ref[...] = high
    low_ref[...] = (weight - high.astype(f32)).astype(bf16)


def dispatch(routing, gate_weights, tokens, slots):
    top, rows = routing.shape
    return pl.pallas_call(
        dispatch_kernel,
        out_shape=(
            jax.ShapeDtypeStruct((slots, tokens.shape[1]), bf16),
            jax.ShapeDtypeStruct((slots, rows), bf16),
            jax.ShapeDtypeStruct((slots, rows), bf16),
        ),
        in_specs=[VMEM] * 3,
        out_specs=(VMEM,) * 3,
        name="dispatch",
    )(routing, gate_weights, tokens)


def order_key(index):
    local = (index // CAP) % 2
    source = index // (2 * CAP)
    return local * 4096 + source * CAP + index % CAP


def order_kernel(received_ref, column_ref, row_ref, count_ref):
    slots, width = received_ref.shape
    filled = received_ref[...].astype(f32) < FILLED_BELOW
    ones = jnp.where(filled, 1.0, 0.0).astype(bf16)
    key_0 = order_key(iota((slots, slots), 0))
    key_1 = order_key(iota((slots, slots), 1))
    column = dot((key_1 < key_0).astype(f32).astype(bf16), ones)
    column = jnp.where(filled, column, -1.0)
    column_ref[...] = column
    across = lax.dot_general(
        jnp.ones((8, width), bf16), ones, (((1,), (1,)), ((), ())), preferred_element_type=f32
    )
    across = jnp.where(across > 0.5, 1.0, 0.0)
    row = dot(across.astype(bf16), (key_0 < key_1).astype(f32).astype(bf16))
    row = jnp.where(across > 0.5, row, -1.0)
    row_ref[...] = row
    total = jnp.max(row).astype(jnp.int32) + 1
    is_first = (iota((8, slots), 1) // CAP) % 2 == 0
    first = jnp.max(jnp.where(is_first, row, -1.0)).astype(jnp.int32) + 1
    bucket = jnp.int32(0)
    for size in BUCKETS[:-1]:
        bucket = bucket + (total > size).astype(jnp.int32)
    count_ref[0] = first
    count_ref[1] = bucket


def order_rows(received):
    slots, width = received.shape
    return pl.pallas_call(
        order_kernel,
        out_shape=(
            jax.ShapeDtypeStruct((slots, width), f32),
            jax.ShapeDtypeStruct((8, slots), f32),
            jax.ShapeDtypeStruct((2,), jnp.int32),
        ),
        in_specs=[VMEM],
        out_specs=(VMEM, VMEM, SMEM),
        name="order_rows",
    )(received)


def compact_kernel(received_ref, row_ref, out_ref):
    copies, size, _ = out_ref.shape
    slots = received_ref.shape[0]
    position = iota((size, slots), 0).astype(f32)
    pick = jnp.where(row_ref[0:1, :] == position, 1.0, 0.0).astype(bf16)
    rows = dot(pick, received_ref[...]).astype(bf16)
    for n in range(copies):
        out_ref[n] = rows


def compact(received, row, copies, size):
    return pl.pallas_call(
        compact_kernel,
        out_shape=jax.ShapeDtypeStruct((copies, size, received.shape[1]), bf16),
        in_specs=[VMEM] * 2,
        out_specs=VMEM,
        name="compact",
    )(received, row)


def expert_kernel(
    count_ref, x_ref, gain_ref, gate_ref, up_ref, down_ref, out_ref, wide, narrow, normed, sems
):
    parts, size, width = x_ref.shape
    copies = []
    for e in range(2):
        for m, ref in enumerate((gate_ref, up_ref)):
            at = (2 * e + m) * width
            copies.append(
                pltpu.make_async_copy(ref.at[e], wide.at[:, at : at + width], sems.at[2 * e + m])
            )
    copies.append(pltpu.make_async_copy(down_ref, narrow, sems.at[4]))
    for copy in copies:
        copy.start()
    ssq = jnp.zeros((size, width), f32)
    for p in range(parts):
        x = x_ref[p].astype(f32)
        ssq = ssq + x * x
    scale = lax.rsqrt(jnp.sum(ssq, axis=1, keepdims=True) / D + norm_eps)
    for p in range(parts):
        x = x_ref[p].astype(f32) * scale * gain_ref[p : p + 1, :]
        normed[:, p * width : (p + 1) * width] = x.astype(bf16)
    for copy in copies[:4]:
        copy.wait()
    pre = dot(normed[...], wide[...])
    row = iota((size, width), 0)
    first = count_ref[0]
    hidden = []
    for e in range(2):
        clamped = jnp.minimum(pre[:, 2 * e * width : (2 * e + 1) * width], clamp_limit)
        upper = jnp.clip(pre[:, (2 * e + 1) * width : (2 * e + 2) * width], -clamp_limit, clamp_limit)
        value = clamped * jax.nn.sigmoid(swish_alpha * clamped) * (upper + 1.0)
        mine = row < first if e == 0 else row >= first
        hidden.append(jnp.where(mine, value, 0.0).astype(bf16))
    hidden = jnp.concatenate(hidden, axis=1)
    copies[4].wait()
    for p in range(0, parts, 2):
        out = dot(hidden, narrow[:, p * width : (p + 2) * width]).astype(bf16)
        out_ref[p] = out[:, :width]
        out_ref[p + 1] = out[:, width:]


def experts(count, x, gain, gate, up, down):
    parts, size, width = x.shape
    return pl.pallas_call(
        expert_kernel,
        out_shape=jax.ShapeDtypeStruct(x.shape, bf16),
        in_specs=[SMEM, VMEM, VMEM, ANY, ANY, ANY],
        out_specs=VMEM,
        scratch_shapes=[
            pltpu.VMEM((D, 4 * width), bf16),
            pltpu.VMEM((2 * width, D), bf16),
            pltpu.VMEM((size, D), bf16),
            pltpu.SemaphoreType.DMA((5,)),
        ],
        name="experts",
    )(count, x, gain, gate, up, down)


def expand_kernel(parts_ref, column_ref, out_ref, total):
    parts, size, width = parts_ref.shape
    slots = column_ref.shape[0]
    padded = total.shape[0]
    value = parts_ref[0].astype(f32)
    for p in range(1, parts):
        value = value + parts_ref[p].astype(f32)
    if padded > size:
        total[...] = jnp.zeros(total.shape, bf16)
    total[:size, :] = value.astype(bf16)
    column = column_ref[...]
    lane = iota((slots, width), 1).astype(f32)
    picks = [
        jnp.where(column == lane + float(b * width), 1.0, 0.0).astype(bf16)
        for b in range(padded // width)
    ]
    out_ref[...] = dot(jnp.concatenate(picks, axis=1), total[...]).astype(bf16)


def expand(parts, column):
    _, size, width = parts.shape
    padded = -(-size // width) * width
    return pl.pallas_call(
        expand_kernel,
        out_shape=jax.ShapeDtypeStruct((column.shape[0], width), bf16),
        in_specs=[VMEM] * 2,
        out_specs=VMEM,
        scratch_shapes=[pltpu.VMEM((padded, width), bf16)],
        name="expand",
    )(parts, column)


def combine_kernel(returned_ref, high_ref, low_ref, out_ref):
    contract = (((0,), (0,)), ((), ()))
    returned = returned_ref[...]
    mixed = lax.dot_general(high_ref[...], returned, contract, preferred_element_type=f32)
    mixed = mixed + lax.dot_general(low_ref[...], returned, contract, preferred_element_type=f32)
    out_ref[...] = mixed.astype(bf16)


def combine(returned, high, low):
    return pl.pallas_call(
        combine_kernel,
        out_shape=jax.ShapeDtypeStruct((high.shape[1], returned.shape[1]), bf16),
        in_specs=[VMEM] * 3,
        out_specs=VMEM,
        name="combine",
    )(returned, high, low)


def exchange(pieces, axis):
    return lax.all_to_all(pieces, axis, split_axis=0, concat_axis=0, tiled=True)


def per_device(tokens, routing, gate_weights, norm_gain, w_gate, w_up, w_down):
    ep_size = lax.axis_size("ep")
    tp_size = lax.axis_size(TP)
    exp_here = w_gate.shape[0]
    width = tokens.shape[1]
    slots = ep_size * exp_here * CAP
    gain = norm_gain.reshape(tp_size, width)
    down = w_down.reshape(exp_here * w_down.shape[1], w_down.shape[2])
    outgoing, high, low = dispatch(routing.T, gate_weights.T, tokens, slots)
    received = exchange(outgoing.reshape(ep_size, exp_here * CAP, width), "ep")
    received = received.reshape(slots, width)
    column, row, count = order_rows(received)

    def middle(size, received, column, row, count, gain, w_gate, w_up, down):
        rows = exchange(compact(received, row, tp_size, size), TP)
        partial_value = experts(count, rows, gain, w_gate, w_up, down)
        return expand(exchange(partial_value, TP), column)

    branches = [functools.partial(middle, size) for size in BUCKETS]
    operands = (received, column, row, count, gain, w_gate, w_up, down)
    if len(branches) == 1:
        back = branches[0](*operands)
    else:
        back = lax.switch(count[1], branches, *operands)
    returned = exchange(back.reshape(ep_size, exp_here * CAP, width), "ep")
    return combine(returned.reshape(slots, width), high, low)


def solution(mesh):
    split = Mesh(mesh.devices.reshape(mesh.shape["ep"], 4, 4), ("ep", "tp_0", "tp_1"))
    placed = (
        P("ep", TP),
        P("ep", None),
        P("ep", None),
        P(),
        P("ep", None, TP),
        P("ep", None, TP),
        P("ep", TP, None),
    )
    return jax.shard_map(
        per_device, mesh=split, in_specs=placed, out_specs=P("ep", TP), check_vma=False
    )
```

```python
import functools

import jax
import jax.numpy as jnp
from jax import lax
from jax.experimental import pallas as pl
from jax.experimental.pallas import tpu as pltpu
from jax.sharding import Mesh
from jax.sharding import PartitionSpec as P

D = 2048
CAP = 8
TP = ("tp_0", "tp_1")
BUCKETS = (144, 208, 272, 352, 416, 512)

norm_eps = 1e-06
clamp_limit = 7.0
swish_alpha = 1.702
EMPTY = 512.0
FILLED_BELOW = 256.0

f32 = jnp.float32
bf16 = jnp.bfloat16
VMEM = pl.BlockSpec(memory_space=pltpu.VMEM)
SMEM = pl.BlockSpec(memory_space=pltpu.SMEM)
ANY = pl.BlockSpec(memory_space=pl.ANY)


def iota(shape, dim):
    return lax.broadcasted_iota(jnp.int32, shape, dim)


def dot(a, b):
    return jnp.dot(a, b, preferred_element_type=f32)


def dispatch_kernel(routing_ref, weight_ref, tokens_ref, out_ref, high_ref, low_ref):
    slots = out_ref.shape[0]
    top, rows = routing_ref.shape
    slot = iota((slots, rows), 0)
    expert = slot // CAP
    chosen = jnp.zeros((slots, rows), f32)
    weight = jnp.zeros((slots, rows), f32)
    for k in range(top):
        match = routing_ref[k : k + 1, :] == expert
        chosen = jnp.where(match, 1.0, chosen)
        weight = jnp.where(match, weight_ref[k : k + 1, :], weight)
    before = (iota((rows, rows), 0) < iota((rows, rows), 1)).astype(f32).astype(bf16)
    rank = dot(chosen.astype(bf16), before).astype(jnp.int32)
    placed = jnp.where(rank == slot % CAP, chosen, 0.0)
    placing = placed.astype(bf16)
    rows_out = dot(placing, tokens_ref[...])
    filled = dot(placing, jnp.ones((rows, out_ref.shape[1]), bf16))
    out_ref[...] = jnp.where(filled > 0.5, rows_out, EMPTY).astype(bf16)
    weight = weight * placed
    high = weight.astype(bf16)
    high_ref[...] = high
    low_ref[...] = (weight - high.astype(f32)).astype(bf16)


def dispatch(routing, gate_weights, tokens, slots):
    top, rows = routing.shape
    return pl.pallas_call(
        dispatch_kernel,
        out_shape=(
            jax.ShapeDtypeStruct((slots, tokens.shape[1]), bf16),
            jax.ShapeDtypeStruct((slots, rows), bf16),
            jax.ShapeDtypeStruct((slots, rows), bf16),
        ),
        in_specs=[VMEM] * 3,
        out_specs=(VMEM,) * 3,
        name="dispatch",
        compiler_params=pltpu.CompilerParams(vmem_limit_bytes=8 << 20),
    )(routing, gate_weights, tokens)


def order_key(index):
    local = (index // CAP) % 2
    source = index // (2 * CAP)
    return local * 4096 + source * CAP + index % CAP


def order_kernel(received_ref, column_ref, row_ref, count_ref):
    slots, width = received_ref.shape
    filled = received_ref[...].astype(f32) < FILLED_BELOW
    ones = jnp.where(filled, 1.0, 0.0).astype(bf16)
    key_0 = order_key(iota((slots, slots), 0))
    key_1 = order_key(iota((slots, slots), 1))
    column = dot((key_1 < key_0).astype(f32).astype(bf16), ones)
    column = jnp.where(filled, column, -1.0)
    column_ref[...] = column
    across = lax.dot_general(
        jnp.ones((8, width), bf16), ones, (((1,), (1,)), ((), ())), preferred_element_type=f32
    )
    across = jnp.where(across > 0.5, 1.0, 0.0)
    row = dot(across.astype(bf16), (key_0 < key_1).astype(f32).astype(bf16))
    row = jnp.where(across > 0.5, row, -1.0)
    row_ref[...] = row
    total = jnp.max(row).astype(jnp.int32) + 1
    is_first = (iota((8, slots), 1) // CAP) % 2 == 0
    first = jnp.max(jnp.where(is_first, row, -1.0)).astype(jnp.int32) + 1
    bucket = jnp.int32(0)
    for size in BUCKETS[:-1]:
        bucket = bucket + (total > size).astype(jnp.int32)
    count_ref[0] = first
    count_ref[1] = bucket


def order_rows(received):
    slots, width = received.shape
    return pl.pallas_call(
        order_kernel,
        out_shape=(
            jax.ShapeDtypeStruct((slots, width), f32),
            jax.ShapeDtypeStruct((8, slots), f32),
            jax.ShapeDtypeStruct((2,), jnp.int32),
        ),
        in_specs=[VMEM],
        out_specs=(VMEM, VMEM, SMEM),
        name="order_rows",
        compiler_params=pltpu.CompilerParams(vmem_limit_bytes=12 << 20),
    )(received)


def compact_kernel(received_ref, row_ref, out_ref):
    copies, size, _ = out_ref.shape
    slots = received_ref.shape[0]
    position = iota((size, slots), 0).astype(f32)
    pick = jnp.where(row_ref[0:1, :] == position, 1.0, 0.0).astype(bf16)
    rows = dot(pick, received_ref[...]).astype(bf16)
    for n in range(copies):
        out_ref[n] = rows


def compact(received, row, copies, size):
    return pl.pallas_call(
        compact_kernel,
        out_shape=jax.ShapeDtypeStruct((copies, size, received.shape[1]), bf16),
        in_specs=[VMEM] * 2,
        out_specs=VMEM,
        name="compact",
        compiler_params=pltpu.CompilerParams(vmem_limit_bytes=12 << 20),
    )(received, row)


def expert_kernel(
    count_ref, x_ref, gain_ref, gate_ref, up_ref, down_ref, out_ref, wide, narrow, normed, sems
):
    parts, size, width = x_ref.shape
    copies = []
    for e in range(2):
        for m, ref in enumerate((gate_ref, up_ref)):
            at = (2 * e + m) * width
            copies.append(
                pltpu.make_async_copy(ref.at[e], wide.at[:, at : at + width], sems.at[2 * e + m])
            )
    copies.append(pltpu.make_async_copy(down_ref, narrow, sems.at[4]))
    for copy in copies:
        copy.start()
    ssq = jnp.zeros((size, width), f32)
    for p in range(parts):
        x = x_ref[p].astype(f32)
        ssq = ssq + x * x
    scale = lax.rsqrt(jnp.sum(ssq, axis=1, keepdims=True) / D + norm_eps)
    for p in range(parts):
        x = x_ref[p].astype(f32) * scale * gain_ref[p : p + 1, :]
        normed[:, p * width : (p + 1) * width] = x.astype(bf16)
    for copy in copies[:4]:
        copy.wait()
    pre = dot(normed[...], wide[...])
    row = iota((size, width), 0)
    first = count_ref[0]
    hidden = []
    for e in range(2):
        clamped = jnp.minimum(pre[:, 2 * e * width : (2 * e + 1) * width], clamp_limit)
        upper = jnp.clip(pre[:, (2 * e + 1) * width : (2 * e + 2) * width], -clamp_limit, clamp_limit)
        value = clamped * jax.nn.sigmoid(swish_alpha * clamped) * (upper + 1.0)
        mine = row < first if e == 0 else row >= first
        hidden.append(jnp.where(mine, value, 0.0).astype(bf16))
    hidden = jnp.concatenate(hidden, axis=1)
    copies[4].wait()
    for p in range(0, parts, 2):
        out = dot(hidden, narrow[:, p * width : (p + 2) * width]).astype(bf16)
        out_ref[p] = out[:, :width]
        out_ref[p + 1] = out[:, width:]


def experts(count, x, gain, gate, up, down):
    parts, size, width = x.shape
    return pl.pallas_call(
        expert_kernel,
        out_shape=jax.ShapeDtypeStruct(x.shape, bf16),
        in_specs=[SMEM, VMEM, VMEM, ANY, ANY, ANY],
        out_specs=VMEM,
        scratch_shapes=[
            pltpu.VMEM((D, 4 * width), bf16),
            pltpu.VMEM((2 * width, D), bf16),
            pltpu.VMEM((size, D), bf16),
            pltpu.SemaphoreType.DMA((5,)),
        ],
        name="experts",
        compiler_params=pltpu.CompilerParams(vmem_limit_bytes=24 << 20),
    )(count, x, gain, gate, up, down)


def expand_kernel(parts_ref, column_ref, out_ref, total):
    parts, size, width = parts_ref.shape
    slots = column_ref.shape[0]
    padded = total.shape[0]
    value = parts_ref[0].astype(f32)
    for p in range(1, parts):
        value = value + parts_ref[p].astype(f32)
    if padded > size:
        total[...] = jnp.zeros(total.shape, bf16)
    total[:size, :] = value.astype(bf16)
    column = column_ref[...]
    lane = iota((slots, width), 1).astype(f32)
    picks = [
        jnp.where(column == lane + float(b * width), 1.0, 0.0).astype(bf16)
        for b in range(padded // width)
    ]
    out_ref[...] = dot(jnp.concatenate(picks, axis=1), total[...]).astype(bf16)


def expand(parts, column):
    _, size, width = parts.shape
    padded = -(-size // width) * width
    return pl.pallas_call(
        expand_kernel,
        out_shape=jax.ShapeDtypeStruct((column.shape[0], width), bf16),
        in_specs=[VMEM] * 2,
        out_specs=VMEM,
        scratch_shapes=[pltpu.VMEM((padded, width), bf16)],
        name="expand",
        compiler_params=pltpu.CompilerParams(vmem_limit_bytes=12 << 20),
    )(parts, column)


def combine_kernel(returned_ref, high_ref, low_ref, out_ref):
    contract = (((0,), (0,)), ((), ()))
    returned = returned_ref[...]
    mixed = lax.dot_general(high_ref[...], returned, contract, preferred_element_type=f32)
    mixed = mixed + lax.dot_general(low_ref[...], returned, contract, preferred_element_type=f32)
    out_ref[...] = mixed.astype(bf16)


def combine(returned, high, low):
    return pl.pallas_call(
        combine_kernel,
        out_shape=jax.ShapeDtypeStruct((high.shape[1], returned.shape[1]), bf16),
        in_specs=[VMEM] * 3,
        out_specs=VMEM,
        name="combine",
        compiler_params=pltpu.CompilerParams(vmem_limit_bytes=8 << 20),
    )(returned, high, low)


def exchange(pieces, axis):
    return lax.all_to_all(pieces, axis, split_axis=0, concat_axis=0, tiled=True)


def per_device(tokens, routing, gate_weights, norm_gain, w_gate, w_up, w_down):
    ep_size = lax.axis_size("ep")
    tp_size = lax.axis_size(TP)
    exp_here = w_gate.shape[0]
    width = tokens.shape[1]
    slots = ep_size * exp_here * CAP
    gain = norm_gain.reshape(tp_size, width)
    down = w_down.reshape(exp_here * w_down.shape[1], w_down.shape[2])
    outgoing, high, low = dispatch(routing.T, gate_weights.T, tokens, slots)
    received = exchange(outgoing.reshape(ep_size, exp_here * CAP, width), "ep")
    received = received.reshape(slots, width)
    column, row, count = order_rows(received)

    def middle(size, received, column, row, count, gain, w_gate, w_up, down):
        rows = exchange(compact(received, row, tp_size, size), TP)
        partial_value = experts(count, rows, gain, w_gate, w_up, down)
        return expand(exchange(partial_value, TP), column)

    branches = [functools.partial(middle, size) for size in BUCKETS]
    operands = (received, column, row, count, gain, w_gate, w_up, down)
    if len(branches) == 1:
        back = branches[0](*operands)
    else:
        back = lax.switch(count[1], branches, *operands)
    returned = exchange(back.reshape(ep_size, exp_here * CAP, width), "ep")
    return combine(returned.reshape(slots, width), high, low)


def solution(mesh):
    split = Mesh(mesh.devices.reshape(mesh.shape["ep"], 4, 4), ("ep", "tp_0", "tp_1"))
    placed = (
        P("ep", TP),
        P("ep", None),
        P("ep", None),
        P(),
        P("ep", None, TP),
        P("ep", None, TP),
        P("ep", TP, None),
    )
    return jax.shard_map(
        per_device, mesh=split, in_specs=placed, out_specs=P("ep", TP), check_vma=False
    )
```

```python
import functools

import jax
import jax.numpy as jnp
from jax import lax
from jax.experimental import pallas as pl
from jax.experimental.pallas import tpu as pltpu
from jax.sharding import Mesh
from jax.sharding import PartitionSpec as P

D = 2048
CAP = 8
TP = ("tp_0", "tp_1")
BUCKETS = (144, 176, 208, 240, 272, 304, 336, 368, 400, 448, 512)

norm_eps = 1e-06
clamp_limit = 7.0
swish_alpha = 1.702
EMPTY = 512.0
FILLED_BELOW = 256.0

f32 = jnp.float32
bf16 = jnp.bfloat16
VMEM = pl.BlockSpec(memory_space=pltpu.VMEM)
SMEM = pl.BlockSpec(memory_space=pltpu.SMEM)


def iota(shape, dim):
    return lax.broadcasted_iota(jnp.int32, shape, dim)


def dot(a, b):
    return jnp.dot(a, b, preferred_element_type=f32)


def place_kernel(routing_ref, placing_ref):
    slots, rows = placing_ref.shape
    slot = iota((slots, rows), 0)
    expert = slot // CAP
    chosen = jnp.zeros((slots, rows), f32)
    for k in range(routing_ref.shape[0]):
        chosen = jnp.where(routing_ref[k : k + 1, :] == expert, 1.0, chosen)
    before = (iota((rows, rows), 0) < iota((rows, rows), 1)).astype(f32).astype(bf16)
    rank = dot(chosen.astype(bf16), before).astype(jnp.int32)
    placing_ref[...] = jnp.where(rank == slot % CAP, chosen, 0.0).astype(bf16)


def place(routing, slots):
    return pl.pallas_call(
        place_kernel,
        out_shape=jax.ShapeDtypeStruct((slots, routing.shape[1]), bf16),
        in_specs=[VMEM],
        out_specs=VMEM,
        name="place",
        cost_estimate=pl.CostEstimate(flops=1 << 29, bytes_accessed=1 << 17, transcendentals=0),
        compiler_params=pltpu.CompilerParams(vmem_limit_bytes=8 << 20),
    )(routing)


def dispatch_kernel(placing_ref, tokens_ref, out_ref):
    placing = placing_ref[...]
    rows = dot(placing, tokens_ref[...])
    filled = dot(placing, jnp.ones(tokens_ref.shape, bf16))
    out_ref[...] = jnp.where(filled > 0.5, rows, EMPTY).astype(bf16)


def dispatch(placing, tokens):
    return pl.pallas_call(
        dispatch_kernel,
        out_shape=jax.ShapeDtypeStruct((placing.shape[0], tokens.shape[1]), bf16),
        in_specs=[VMEM] * 2,
        out_specs=VMEM,
        name="dispatch",
        compiler_params=pltpu.CompilerParams(vmem_limit_bytes=8 << 20),
    )(placing, tokens)


def order_key(index):
    return (index & CAP) * 512 + index


def order_kernel(received_ref, column_ref, row_ref, first_ref, bucket_ref):
    slots, width = received_ref.shape
    filled = received_ref[...].astype(f32) < FILLED_BELOW
    ones = jnp.where(filled, 1.0, 0.0).astype(bf16)
    own_key = order_key(iota((slots, width), 0))
    other_key = order_key(iota((1, slots), 1))
    later = [
        jnp.where(other_key[:, b : b + width] < own_key, 1.0, 0.0).astype(bf16)
        for b in range(0, slots, width)
    ]
    later = jnp.concatenate(later, axis=1)
    column = dot(later, ones)
    column_ref[...] = jnp.where(filled, column, -1.0)
    across = lax.dot_general(
        jnp.full((8, width), 1.0 / width, bf16),
        ones,
        (((1,), (1,)), ((), ())),
        preferred_element_type=f32,
    )
    total = jnp.sum(across[0:1, :], axis=1, keepdims=True)
    row = total - 1.0 - dot(across.astype(bf16), later)
    row_ref[...] = jnp.where(across > 0.5, row, -1.0)
    is_first = (iota((1, slots), 1) & CAP) == 0
    first = jnp.sum(jnp.where(is_first, across[0:1, :], 0.0))
    count = jnp.sum(across[0:1, :])
    bucket = jnp.int32(0)
    for size in BUCKETS[:-1]:
        bucket = bucket + (count > size).astype(jnp.int32)
    first_ref[0] = first.astype(jnp.int32)
    bucket_ref[0] = bucket


def order_rows(received):
    slots, width = received.shape
    return pl.pallas_call(
        order_kernel,
        out_shape=(
            jax.ShapeDtypeStruct((slots, width), f32),
            jax.ShapeDtypeStruct((8, slots), f32),
            jax.ShapeDtypeStruct((1,), jnp.int32),
            jax.ShapeDtypeStruct((1,), jnp.int32),
        ),
        in_specs=[VMEM],
        out_specs=(VMEM, VMEM, SMEM, SMEM),
        name="order_rows",
        compiler_params=pltpu.CompilerParams(vmem_limit_bytes=12 << 20),
    )(received)


def compact_kernel(received_ref, row_ref, out_ref):
    copies, size, _ = out_ref.shape
    slots = received_ref.shape[0]
    position = iota((size, slots), 0).astype(f32)
    pick = jnp.where(row_ref[0:1, :] == position, 1.0, 0.0).astype(bf16)
    rows = dot(pick, received_ref[...]).astype(bf16)
    for n in range(copies):
        out_ref[n] = rows


def compact(received, row, copies, size):
    return pl.pallas_call(
        compact_kernel,
        out_shape=jax.ShapeDtypeStruct((copies, size, received.shape[1]), bf16),
        in_specs=[VMEM] * 2,
        out_specs=VMEM,
        name="compact",
        compiler_params=pltpu.CompilerParams(vmem_limit_bytes=12 << 20),
    )(received, row)


def expert_kernel(first_ref, x_ref, gain_ref, gate_ref, up_ref, down_ref, out_ref, normed):
    parts, size, width = x_ref.shape
    ssq = jnp.zeros((size, width), f32)
    for p in range(parts):
        x = x_ref[p].astype(f32)
        ssq = ssq + x * x
    scale = lax.rsqrt(jnp.sum(ssq, axis=1, keepdims=True) / D + norm_eps)
    for p in range(parts):
        x = x_ref[p].astype(f32) * scale * gain_ref[p : p + 1, :]
        normed[:, p * width : (p + 1) * width] = x.astype(bf16)
    row = iota((size, width), 0)
    first = first_ref[0]
    hidden = []
    for e in range(2):
        pre = dot(normed[...], jnp.concatenate([gate_ref[e], up_ref[e]], axis=1))
        clamped = jnp.minimum(pre[:, :width], clamp_limit)
        upper = jnp.clip(pre[:, width:], -clamp_limit, clamp_limit)
        value = clamped * jax.nn.sigmoid(swish_alpha * clamped) * (upper + 1.0)
        mine = row < first if e == 0 else row >= first
        hidden.append(jnp.where(mine, value, 0.0).astype(bf16))
    hidden = jnp.concatenate(hidden, axis=1)
    for p in range(0, parts, 2):
        out = dot(hidden, down_ref[:, p * width : (p + 2) * width]).astype(bf16)
        out_ref[p] = out[:, :width]
        out_ref[p + 1] = out[:, width:]


def experts(first, x, gain, gate, up, down):
    parts, size, width = x.shape
    return pl.pallas_call(
        expert_kernel,
        out_shape=jax.ShapeDtypeStruct(x.shape, bf16),
        in_specs=[SMEM] + [VMEM] * 5,
        out_specs=VMEM,
        scratch_shapes=[pltpu.VMEM((size, D), bf16)],
        name="experts",
        compiler_params=pltpu.CompilerParams(vmem_limit_bytes=20 << 20),
    )(first, x, gain, gate, up, down)


def expand_kernel(parts_ref, column_ref, out_ref, total):
    parts, size, width = parts_ref.shape
    slots = column_ref.shape[0]
    padded = total.shape[0]
    value = parts_ref[0].astype(f32)
    for p in range(1, parts):
        value = value + parts_ref[p].astype(f32)
    if padded > size:
        total[...] = jnp.zeros(total.shape, bf16)
    total[:size, :] = value.astype(bf16)
    column = column_ref[...]
    lane = iota((slots, width), 1).astype(f32)
    picks = [
        jnp.where(column == lane + float(b * width), 1.0, 0.0).astype(bf16)
        for b in range(padded // width)
    ]
    out_ref[...] = dot(jnp.concatenate(picks, axis=1), total[...]).astype(bf16)


def expand(parts, column):
    _, size, width = parts.shape
    padded = -(-size // width) * width
    return pl.pallas_call(
        expand_kernel,
        out_shape=jax.ShapeDtypeStruct((column.shape[0], width), bf16),
        in_specs=[VMEM] * 2,
        out_specs=VMEM,
        scratch_shapes=[pltpu.VMEM((padded, width), bf16)],
        name="expand",
        compiler_params=pltpu.CompilerParams(vmem_limit_bytes=12 << 20),
    )(parts, column)


def combine_kernel(returned_ref, placing_ref, routing_ref, weight_ref, out_ref):
    slots, rows = placing_ref.shape
    expert = iota((slots, rows), 0) // CAP
    weight = jnp.zeros((slots, rows), f32)
    for k in range(routing_ref.shape[0]):
        weight = jnp.where(routing_ref[k : k + 1, :] == expert, weight_ref[k : k + 1, :], weight)
    weight = weight * placing_ref[...].astype(f32)
    high = weight.astype(bf16)
    low = (weight - high.astype(f32)).astype(bf16)
    contract = (((0,), (0,)), ((), ()))
    returned = returned_ref[...]
    mixed = lax.dot_general(high, returned, contract, preferred_element_type=f32)
    mixed = mixed + lax.dot_general(low, returned, contract, preferred_element_type=f32)
    out_ref[...] = mixed.astype(bf16)


def combine(returned, placing, routing, gate_weights):
    return pl.pallas_call(
        combine_kernel,
        out_shape=jax.ShapeDtypeStruct((placing.shape[1], returned.shape[1]), bf16),
        in_specs=[VMEM] * 4,
        out_specs=VMEM,
        name="combine",
        compiler_params=pltpu.CompilerParams(vmem_limit_bytes=8 << 20),
    )(returned, placing, routing, gate_weights)


def exchange(pieces, axis):
    return lax.all_to_all(pieces, axis, split_axis=0, concat_axis=0, tiled=True)


def per_device(tokens, routing, gate_weights, norm_gain, w_gate, w_up, w_down):
    ep_size = lax.axis_size("ep")
    tp_size = lax.axis_size(TP)
    exp_here = w_gate.shape[0]
    width = tokens.shape[1]
    slots = ep_size * exp_here * CAP
    gain = norm_gain.reshape(tp_size, width)
    down = w_down.reshape(exp_here * w_down.shape[1], w_down.shape[2])
    placing = place(routing.T, slots)
    outgoing = dispatch(placing, tokens)
    received = exchange(outgoing.reshape(ep_size, exp_here * CAP, width), "ep")
    received = received.reshape(slots, width)
    column, row, first, bucket = order_rows(received)

    def middle(size, received, column, row, first, gain, w_gate, w_up, down):
        rows = exchange(compact(received, row, tp_size, size), TP)
        partial_value = experts(first, rows, gain, w_gate, w_up, down)
        return expand(exchange(partial_value, TP), column)

    branches = [functools.partial(middle, size) for size in BUCKETS]
    operands = (received, column, row, first, gain, w_gate, w_up, down)
    if len(branches) == 1:
        back = branches[0](*operands)
    else:
        back = lax.switch(bucket[0], branches, *operands)
    returned = exchange(back.reshape(ep_size, exp_here * CAP, width), "ep")
    return combine(returned.reshape(slots, width), placing, routing.T, gate_weights.T)


def solution(mesh):
    split = Mesh(mesh.devices.reshape(mesh.shape["ep"], 4, 4), ("ep", "tp_0", "tp_1"))
    placed = (
        P("ep", TP),
        P("ep", None),
        P("ep", None),
        P(),
        P("ep", None, TP),
        P("ep", None, TP),
        P("ep", TP, None),
    )
    return jax.shard_map(
        per_device, mesh=split, in_specs=placed, out_specs=P("ep", TP), check_vma=False
    )
```

```python
import functools

import jax
import jax.numpy as jnp
from jax import lax
from jax.experimental import pallas as pl
from jax.experimental.pallas import tpu as pltpu
from jax.sharding import Mesh
from jax.sharding import PartitionSpec as P

D = 2048
CAP = 8
TP = ("tp_0", "tp_1")
BUCKETS = (144, 176, 208, 240, 272, 304, 336, 368, 400, 448, 512)

norm_eps = 1e-06
clamp_limit = 7.0
swish_alpha = 1.702
EMPTY = 512.0
FILLED_BELOW = 256.0

TP_ORDER = [0, 1, 2, 3, 7, 4, 5, 6, 10, 11, 8, 9, 13, 14, 15, 12]

f32 = jnp.float32
bf16 = jnp.bfloat16
VMEM = pl.BlockSpec(memory_space=pltpu.VMEM)
SMEM = pl.BlockSpec(memory_space=pltpu.SMEM)


def iota(shape, dim):
    return lax.broadcasted_iota(jnp.int32, shape, dim)


def dot(a, b):
    return jnp.dot(a, b, preferred_element_type=f32)


def place_kernel(routing_ref, placing_ref):
    slots, rows = placing_ref.shape
    slot = iota((slots, rows), 0)
    expert = slot // CAP
    chosen = jnp.zeros((slots, rows), f32)
    for k in range(routing_ref.shape[0]):
        chosen = jnp.where(routing_ref[k : k + 1, :] == expert, 1.0, chosen)
    before = (iota((rows, rows), 0) < iota((rows, rows), 1)).astype(f32).astype(bf16)
    rank = dot(chosen.astype(bf16), before).astype(jnp.int32)
    placing_ref[...] = jnp.where(rank == slot % CAP, chosen, 0.0).astype(bf16)


def place(routing, slots):
    return pl.pallas_call(
        place_kernel,
        out_shape=jax.ShapeDtypeStruct((slots, routing.shape[1]), bf16),
        in_specs=[VMEM],
        out_specs=VMEM,
        name="place",
        cost_estimate=pl.CostEstimate(flops=1 << 29, bytes_accessed=1 << 17, transcendentals=0),
        compiler_params=pltpu.CompilerParams(vmem_limit_bytes=8 << 20),
    )(routing)


def dispatch_kernel(placing_ref, tokens_ref, out_ref):
    placing = placing_ref[...]
    rows = dot(placing, tokens_ref[...])
    filled = dot(placing, jnp.ones(tokens_ref.shape, bf16))
    out_ref[...] = jnp.where(filled > 0.5, rows, EMPTY).astype(bf16)


def dispatch(placing, tokens):
    return pl.pallas_call(
        dispatch_kernel,
        out_shape=jax.ShapeDtypeStruct((placing.shape[0], tokens.shape[1]), bf16),
        in_specs=[VMEM] * 2,
        out_specs=VMEM,
        name="dispatch",
        compiler_params=pltpu.CompilerParams(vmem_limit_bytes=8 << 20),
    )(placing, tokens)


def order_key(index):
    return (index & CAP) * 512 + index


def order_kernel(received_ref, column_ref, row_ref, first_ref, bucket_ref):
    slots, width = received_ref.shape
    filled = received_ref[...].astype(f32) < FILLED_BELOW
    ones = jnp.where(filled, 1.0, 0.0).astype(bf16)
    own_key = order_key(iota((slots, width), 0))
    other_key = order_key(iota((1, slots), 1))
    later = [
        jnp.where(other_key[:, b : b + width] < own_key, 1.0, 0.0).astype(bf16)
        for b in range(0, slots, width)
    ]
    later = jnp.concatenate(later, axis=1)
    column = dot(later, ones)
    column_ref[...] = jnp.where(filled, column, -1.0)
    across = lax.dot_general(
        jnp.full((8, width), 1.0 / width, bf16),
        ones,
        (((1,), (1,)), ((), ())),
        preferred_element_type=f32,
    )
    total = jnp.sum(across[0:1, :], axis=1, keepdims=True)
    row = total - 1.0 - dot(across.astype(bf16), later)
    row_ref[...] = jnp.where(across > 0.5, row, -1.0)
    is_first = (iota((1, slots), 1) & CAP) == 0
    first = jnp.sum(jnp.where(is_first, across[0:1, :], 0.0), axis=1, keepdims=True)
    count = jnp.sum(across[0:1, :])
    bucket = jnp.int32(0)
    for size in BUCKETS[:-1]:
        bucket = bucket + (count > size).astype(jnp.int32)
    first_ref[...] = jnp.zeros(first_ref.shape, f32) + first
    bucket_ref[0] = bucket


def order_rows(received):
    slots, width = received.shape
    return pl.pallas_call(
        order_kernel,
        out_shape=(
            jax.ShapeDtypeStruct((slots, width), f32),
            jax.ShapeDtypeStruct((8, slots), f32),
            jax.ShapeDtypeStruct((8, width), f32),
            jax.ShapeDtypeStruct((1,), jnp.int32),
        ),
        in_specs=[VMEM],
        out_specs=(VMEM, VMEM, VMEM, SMEM),
        name="order_rows",
        compiler_params=pltpu.CompilerParams(vmem_limit_bytes=12 << 20),
    )(received)


def compact_kernel(received_ref, row_ref, out_ref):
    copies, size, _ = out_ref.shape
    slots = received_ref.shape[0]
    position = iota((size, slots), 0).astype(f32)
    pick = jnp.where(row_ref[0:1, :] == position, 1.0, 0.0).astype(bf16)
    rows = dot(pick, received_ref[...]).astype(bf16)
    for n in range(copies):
        out_ref[n] = rows


def compact(received, row, copies, size):
    return pl.pallas_call(
        compact_kernel,
        out_shape=jax.ShapeDtypeStruct((copies, size, received.shape[1]), bf16),
        in_specs=[VMEM] * 2,
        out_specs=VMEM,
        name="compact",
        compiler_params=pltpu.CompilerParams(vmem_limit_bytes=12 << 20),
    )(received, row)


def expert_kernel(first_ref, x_ref, gain_ref, gate_ref, up_ref, down_ref, out_ref, normed):
    parts, size, width = x_ref.shape
    ssq = jnp.zeros((size, width), f32)
    for p in range(parts):
        x = x_ref[p].astype(f32)
        ssq = ssq + x * x
    scale = lax.rsqrt(jnp.sum(ssq, axis=1, keepdims=True) / D + norm_eps)
    for p in range(parts):
        q = TP_ORDER[p]
        x = x_ref[p].astype(f32) * scale * gain_ref[q : q + 1, :]
        normed[:, q * width : (q + 1) * width] = x.astype(bf16)
    row = iota((size, width), 0).astype(f32)
    first = first_ref[0:1, :]
    hidden = []
    for e in range(2):
        pre = dot(normed[...], jnp.concatenate([gate_ref[e], up_ref[e]], axis=1))
        clamped = jnp.minimum(pre[:, :width], clamp_limit)
        upper = jnp.clip(pre[:, width:], -clamp_limit, clamp_limit)
        value = clamped * jax.nn.sigmoid(swish_alpha * clamped) * (upper + 1.0)
        mine = row < first if e == 0 else row >= first
        hidden.append(jnp.where(mine, value, 0.0).astype(bf16))
    hidden = jnp.concatenate(hidden, axis=1)
    for p in range(0, parts, 2):
        out = dot(hidden, down_ref[:, p * width : (p + 2) * width]).astype(bf16)
        out_ref[TP_ORDER.index(p)] = out[:, :width]
        out_ref[TP_ORDER.index(p + 1)] = out[:, width:]


def experts(first, x, gain, gate, up, down):
    parts, size, width = x.shape
    return pl.pallas_call(
        expert_kernel,
        out_shape=jax.ShapeDtypeStruct(x.shape, bf16),
        in_specs=[VMEM] * 6,
        out_specs=VMEM,
        scratch_shapes=[pltpu.VMEM((size, D), bf16)],
        name="experts",
        compiler_params=pltpu.CompilerParams(vmem_limit_bytes=20 << 20),
    )(first, x, gain, gate, up, down)


def expand_kernel(parts_ref, column_ref, out_ref, total):
    parts, size, width = parts_ref.shape
    slots = column_ref.shape[0]
    padded = total.shape[0]
    value = parts_ref[0].astype(f32)
    for p in range(1, parts):
        value = value + parts_ref[p].astype(f32)
    if padded > size:
        total[...] = jnp.zeros(total.shape, bf16)
    total[:size, :] = value.astype(bf16)
    column = column_ref[...]
    lane = iota((slots, width), 1).astype(f32)
    picks = [
        jnp.where(column == lane + float(b * width), 1.0, 0.0).astype(bf16)
        for b in range(padded // width)
    ]
    out_ref[...] = dot(jnp.concatenate(picks, axis=1), total[...]).astype(bf16)


def expand(parts, column):
    _, size, width = parts.shape
    padded = -(-size // width) * width
    return pl.pallas_call(
        expand_kernel,
        out_shape=jax.ShapeDtypeStruct((column.shape[0], width), bf16),
        in_specs=[VMEM] * 2,
        out_specs=VMEM,
        scratch_shapes=[pltpu.VMEM((padded, width), bf16)],
        name="expand",
        compiler_params=pltpu.CompilerParams(vmem_limit_bytes=12 << 20),
    )(parts, column)


def combine_kernel(returned_ref, placing_ref, routing_ref, weight_ref, out_ref):
    slots, rows = placing_ref.shape
    expert = iota((slots, rows), 0) // CAP
    weight = jnp.zeros((slots, rows), f32)
    for k in range(routing_ref.shape[0]):
        weight = jnp.where(routing_ref[k : k + 1, :] == expert, weight_ref[k : k + 1, :], weight)
    weight = weight * placing_ref[...].astype(f32)
    high = weight.astype(bf16)
    low = (weight - high.astype(f32)).astype(bf16)
    contract = (((0,), (0,)), ((), ()))
    returned = returned_ref[...]
    mixed = lax.dot_general(high, returned, contract, preferred_element_type=f32)
    mixed = mixed + lax.dot_general(low, returned, contract, preferred_element_type=f32)
    out_ref[...] = mixed.astype(bf16)


def combine(returned, placing, routing, gate_weights):
    return pl.pallas_call(
        combine_kernel,
        out_shape=jax.ShapeDtypeStruct((placing.shape[1], returned.shape[1]), bf16),
        in_specs=[VMEM] * 4,
        out_specs=VMEM,
        name="combine",
        compiler_params=pltpu.CompilerParams(vmem_limit_bytes=8 << 20),
    )(returned, placing, routing, gate_weights)


def exchange(pieces, axis, order=None):
    groups = None if order is None else [order]
    return lax.all_to_all(
        pieces, axis, split_axis=0, concat_axis=0, axis_index_groups=groups, tiled=True
    )


def per_device(tokens, routing, gate_weights, norm_gain, w_gate, w_up, w_down):
    ep_size = lax.axis_size("ep")
    tp_size = lax.axis_size(TP)
    exp_here = w_gate.shape[0]
    width = tokens.shape[1]
    slots = ep_size * exp_here * CAP
    gain = norm_gain.reshape(tp_size, width)
    down = w_down.reshape(exp_here * w_down.shape[1], w_down.shape[2])
    placing = place(routing.T, slots)
    outgoing = dispatch(placing, tokens)
    received = exchange(outgoing.reshape(ep_size, exp_here * CAP, width), "ep")
    received = received.reshape(slots, width)
    column, row, first, bucket = order_rows(received)

    def middle(size, received, column, row, first, gain, w_gate, w_up, down):
        rows = exchange(compact(received, row, tp_size, size), TP, TP_ORDER)
        partial_value = experts(first, rows, gain, w_gate, w_up, down)
        return expand(exchange(partial_value, TP, TP_ORDER), column)

    branches = [functools.partial(middle, size) for size in BUCKETS]
    operands = (received, column, row, first, gain, w_gate, w_up, down)
    if len(branches) == 1:
        back = branches[0](*operands)
    else:
        back = lax.switch(bucket[0], branches, *operands)
    returned = exchange(back.reshape(ep_size, exp_here * CAP, width), "ep")
    return combine(returned.reshape(slots, width), placing, routing.T, gate_weights.T)


def solution(mesh):
    split = Mesh(mesh.devices.reshape(mesh.shape["ep"], 4, 4), ("ep", "tp_0", "tp_1"))
    placed = (
        P("ep", TP),
        P("ep", None),
        P("ep", None),
        P(),
        P("ep", None, TP),
        P("ep", None, TP),
        P("ep", TP, None),
    )
    return jax.shard_map(
        per_device, mesh=split, in_specs=placed, out_specs=P("ep", TP), check_vma=False
    )
```

```python
import functools

import jax
import jax.numpy as jnp
from jax import lax
from jax.experimental import pallas as pl
from jax.experimental.pallas import tpu as pltpu
from jax.sharding import Mesh
from jax.sharding import PartitionSpec as P

D = 2048
CAP = 8
TP = ("tp_0", "tp_1")
BUCKETS = (144, 176, 208, 240, 272, 304, 336, 368, 400, 448, 512)

norm_eps = 1e-06
clamp_limit = 7.0
swish_alpha = 1.702
EMPTY = 512.0
FILLED_BELOW = 256.0

TP_ORDER = [0, 1, 2, 3, 7, 4, 5, 6, 10, 11, 8, 9, 13, 14, 15, 12]

f32 = jnp.float32
bf16 = jnp.bfloat16
VMEM = pl.BlockSpec(memory_space=pltpu.VMEM)
SMEM = pl.BlockSpec(memory_space=pltpu.SMEM)


def iota(shape, dim):
    return lax.broadcasted_iota(jnp.int32, shape, dim)


def dot(a, b):
    return jnp.dot(a, b, preferred_element_type=f32)


def place_kernel(routing_ref, placing_ref):
    slots, rows = placing_ref.shape
    slot = iota((slots, rows), 0)
    expert = slot // CAP
    chosen = jnp.zeros((slots, rows), f32)
    for k in range(routing_ref.shape[0]):
        chosen = jnp.where(routing_ref[k : k + 1, :] == expert, 1.0, chosen)
    before = (iota((rows, rows), 0) < iota((rows, rows), 1)).astype(f32).astype(bf16)
    rank = dot(chosen.astype(bf16), before).astype(jnp.int32)
    placing_ref[...] = jnp.where(rank == slot % CAP, chosen, 0.0).astype(bf16)


def place(routing, slots):
    return pl.pallas_call(
        place_kernel,
        out_shape=jax.ShapeDtypeStruct((slots, routing.shape[1]), bf16),
        in_specs=[VMEM],
        out_specs=VMEM,
        name="place",
        cost_estimate=pl.CostEstimate(flops=1 << 29, bytes_accessed=1 << 17, transcendentals=0),
        compiler_params=pltpu.CompilerParams(vmem_limit_bytes=8 << 20),
    )(routing)


def dispatch_kernel(placing_ref, tokens_ref, out_ref):
    placing = placing_ref[...]
    rows = dot(placing, tokens_ref[...])
    filled = dot(placing, jnp.ones(tokens_ref.shape, bf16))
    out_ref[...] = jnp.where(filled > 0.5, rows, EMPTY).astype(bf16)


def dispatch(placing, tokens):
    return pl.pallas_call(
        dispatch_kernel,
        out_shape=jax.ShapeDtypeStruct((placing.shape[0], tokens.shape[1]), bf16),
        in_specs=[VMEM] * 2,
        out_specs=VMEM,
        name="dispatch",
        compiler_params=pltpu.CompilerParams(vmem_limit_bytes=8 << 20),
    )(placing, tokens)


def order_key(index):
    return (index & CAP) * 512 + index


def order_kernel(received_ref, column_ref, row_ref, first_ref, bucket_ref):
    slots, width = received_ref.shape
    filled = received_ref[...].astype(f32) < FILLED_BELOW
    ones = jnp.where(filled, 1.0, 0.0).astype(bf16)
    own_key = order_key(iota((slots, width), 0))
    other_key = order_key(iota((1, slots), 1))
    later = [
        jnp.where(other_key[:, b : b + width] < own_key, 1.0, 0.0).astype(bf16)
        for b in range(0, slots, width)
    ]
    later = jnp.concatenate(later, axis=1)
    column = dot(later, ones)
    column_ref[...] = jnp.where(filled, column, -1.0)
    across = lax.dot_general(
        jnp.full((8, width), 1.0 / width, bf16),
        ones,
        (((1,), (1,)), ((), ())),
        preferred_element_type=f32,
    )
    total = jnp.sum(across[0:1, :], axis=1, keepdims=True)
    row = total - 1.0 - dot(across.astype(bf16), later)
    row_ref[...] = jnp.where(across > 0.5, row, -1.0)
    is_first = (iota((1, slots), 1) & CAP) == 0
    first = jnp.sum(jnp.where(is_first, across[0:1, :], 0.0), axis=1, keepdims=True)
    count = jnp.sum(across[0:1, :])
    bucket = jnp.int32(0)
    for size in BUCKETS[:-1]:
        bucket = bucket + (count > size).astype(jnp.int32)
    first_ref[...] = jnp.zeros(first_ref.shape, f32) + first
    bucket_ref[0] = bucket


def order_rows(received):
    slots, width = received.shape
    return pl.pallas_call(
        order_kernel,
        out_shape=(
            jax.ShapeDtypeStruct((slots, width), f32),
            jax.ShapeDtypeStruct((8, slots), f32),
            jax.ShapeDtypeStruct((8, width), f32),
            jax.ShapeDtypeStruct((1,), jnp.int32),
        ),
        in_specs=[VMEM],
        out_specs=(VMEM, VMEM, VMEM, SMEM),
        name="order_rows",
        compiler_params=pltpu.CompilerParams(vmem_limit_bytes=12 << 20),
    )(received)


def compact_kernel(received_ref, row_ref, gain_ref, out_ref):
    copies, size, _ = out_ref.shape
    slots = received_ref.shape[0]
    position = iota((size, slots), 0).astype(f32)
    pick = jnp.where(row_ref[0:1, :] == position, 1.0, 0.0).astype(bf16)
    gain = gain_ref[pl.ds(lax.axis_index(TP), 1), :]
    rows = (dot(pick, received_ref[...]) * gain).astype(bf16)
    for n in range(copies):
        out_ref[n] = rows


def compact(received, row, gain, size):
    copies = gain.shape[0]
    return pl.pallas_call(
        compact_kernel,
        out_shape=jax.ShapeDtypeStruct((copies, size, received.shape[1]), bf16),
        in_specs=[VMEM] * 3,
        out_specs=VMEM,
        name="compact",
        compiler_params=pltpu.CompilerParams(vmem_limit_bytes=12 << 20),
    )(received, row, gain)


def expert_kernel(first_ref, x_ref, gain_ref, gate_ref, up_ref, down_ref, out_ref):
    parts, size, width = x_ref.shape
    undo = 1.0 / (gain_ref[...] * gain_ref[...])
    ssq = jnp.zeros((size, width), f32)
    for p in range(parts):
        x = x_ref[p].astype(f32)
        q = TP_ORDER[p]
        ssq = ssq + x * x * undo[q : q + 1, :]
    scale = lax.rsqrt(jnp.sum(ssq, axis=1, keepdims=True) / D + norm_eps)
    rows = jnp.concatenate([x_ref[TP_ORDER.index(q)] for q in range(parts)], axis=1)
    row = iota((size, width), 0).astype(f32)
    first = first_ref[0:1, :]
    hidden = []
    for e in range(2):
        pre = dot(rows, jnp.concatenate([gate_ref[e], up_ref[e]], axis=1)) * scale
        clamped = jnp.minimum(pre[:, :width], clamp_limit)
        upper = jnp.clip(pre[:, width:], -clamp_limit, clamp_limit)
        value = clamped * jax.nn.sigmoid(swish_alpha * clamped) * (upper + 1.0)
        mine = row < first if e == 0 else row >= first
        hidden.append(jnp.where(mine, value, 0.0).astype(bf16))
    hidden = jnp.concatenate(hidden, axis=1)
    for p in range(0, parts, 2):
        out = dot(hidden, down_ref[:, p * width : (p + 2) * width]).astype(bf16)
        out_ref[TP_ORDER.index(p)] = out[:, :width]
        out_ref[TP_ORDER.index(p + 1)] = out[:, width:]


def experts(first, x, gain, gate, up, down):
    parts, size, width = x.shape
    return pl.pallas_call(
        expert_kernel,
        out_shape=jax.ShapeDtypeStruct(x.shape, bf16),
        in_specs=[VMEM] * 6,
        out_specs=VMEM,
        name="experts",
        compiler_params=pltpu.CompilerParams(vmem_limit_bytes=20 << 20),
    )(first, x, gain, gate, up, down)


def expand_kernel(parts_ref, column_ref, out_ref, total):
    parts, size, width = parts_ref.shape
    slots = column_ref.shape[0]
    padded = total.shape[0]
    value = parts_ref[0].astype(f32)
    for p in range(1, parts):
        value = value + parts_ref[p].astype(f32)
    if padded > size:
        total[...] = jnp.zeros(total.shape, bf16)
    total[:size, :] = value.astype(bf16)
    column = column_ref[...]
    lane = iota((slots, width), 1).astype(f32)
    picks = [
        jnp.where(column == lane + float(b * width), 1.0, 0.0).astype(bf16)
        for b in range(padded // width)
    ]
    out_ref[...] = dot(jnp.concatenate(picks, axis=1), total[...]).astype(bf16)


def expand(parts, column):
    _, size, width = parts.shape
    padded = -(-size // width) * width
    return pl.pallas_call(
        expand_kernel,
        out_shape=jax.ShapeDtypeStruct((column.shape[0], width), bf16),
        in_specs=[VMEM] * 2,
        out_specs=VMEM,
        scratch_shapes=[pltpu.VMEM((padded, width), bf16)],
        name="expand",
        compiler_params=pltpu.CompilerParams(vmem_limit_bytes=12 << 20),
    )(parts, column)


def combine_kernel(returned_ref, placing_ref, routing_ref, weight_ref, out_ref):
    slots, rows = placing_ref.shape
    expert = iota((slots, rows), 0) // CAP
    weight = jnp.zeros((slots, rows), f32)
    for k in range(routing_ref.shape[0]):
        weight = jnp.where(routing_ref[k : k + 1, :] == expert, weight_ref[k : k + 1, :], weight)
    weight = weight * placing_ref[...].astype(f32)
    high = weight.astype(bf16)
    low = (weight - high.astype(f32)).astype(bf16)
    contract = (((0,), (0,)), ((), ()))
    returned = returned_ref[...]
    mixed = lax.dot_general(high, returned, contract, preferred_element_type=f32)
    mixed = mixed + lax.dot_general(low, returned, contract, preferred_element_type=f32)
    out_ref[...] = mixed.astype(bf16)


def combine(returned, placing, routing, gate_weights):
    return pl.pallas_call(
        combine_kernel,
        out_shape=jax.ShapeDtypeStruct((placing.shape[1], returned.shape[1]), bf16),
        in_specs=[VMEM] * 4,
        out_specs=VMEM,
        name="combine",
        compiler_params=pltpu.CompilerParams(vmem_limit_bytes=8 << 20),
    )(returned, placing, routing, gate_weights)


def exchange(pieces, axis, order=None):
    groups = None if order is None else [order]
    return lax.all_to_all(
        pieces, axis, split_axis=0, concat_axis=0, axis_index_groups=groups, tiled=True
    )


def per_device(tokens, routing, gate_weights, norm_gain, w_gate, w_up, w_down):
    ep_size = lax.axis_size("ep")
    tp_size = lax.axis_size(TP)
    exp_here = w_gate.shape[0]
    width = tokens.shape[1]
    slots = ep_size * exp_here * CAP
    gain = norm_gain.reshape(tp_size, width)
    down = w_down.reshape(exp_here * w_down.shape[1], w_down.shape[2])
    placing = place(routing.T, slots)
    outgoing = dispatch(placing, tokens)
    received = exchange(outgoing.reshape(ep_size, exp_here * CAP, width), "ep")
    received = received.reshape(slots, width)
    column, row, first, bucket = order_rows(received)

    def middle(size, received, column, row, first, gain, w_gate, w_up, down):
        rows = exchange(compact(received, row, gain, size), TP, TP_ORDER)
        partial_value = experts(first, rows, gain, w_gate, w_up, down)
        return expand(exchange(partial_value, TP, TP_ORDER), column)

    branches = [functools.partial(middle, size) for size in BUCKETS]
    operands = (received, column, row, first, gain, w_gate, w_up, down)
    if len(branches) == 1:
        back = branches[0](*operands)
    else:
        back = lax.switch(bucket[0], branches, *operands)
    returned = exchange(back.reshape(ep_size, exp_here * CAP, width), "ep")
    return combine(returned.reshape(slots, width), placing, routing.T, gate_weights.T)


def solution(mesh):
    split = Mesh(mesh.devices.reshape(mesh.shape["ep"], 4, 4), ("ep", "tp_0", "tp_1"))
    placed = (
        P("ep", TP),
        P("ep", None),
        P("ep", None),
        P(),
        P("ep", None, TP),
        P("ep", None, TP),
        P("ep", TP, None),
    )
    return jax.shard_map(
        per_device, mesh=split, in_specs=placed, out_specs=P("ep", TP), check_vma=False
    )
```

```python
import functools

import jax
import jax.numpy as jnp
from jax import lax
from jax.experimental import pallas as pl
from jax.experimental.pallas import tpu as pltpu
from jax.sharding import Mesh
from jax.sharding import PartitionSpec as P

D = 2048
CAP = 8
TP = ("tp_0", "tp_1")
BUCKETS = (144, 176, 208, 240, 272, 304, 336, 368, 400, 448, 512)

norm_eps = 1e-06
clamp_limit = 7.0
swish_alpha = 1.702
EMPTY = 512.0
FILLED_BELOW = 256.0

TP_ORDER = [10, 11, 8, 9, 13, 14, 15, 12, 0, 1, 2, 3, 7, 4, 5, 6]
TP_BACK_ORDER = [10, 11, 8, 9, 13, 14, 15, 12, 0, 1, 2, 3, 7, 4, 5, 6]

CHIPS = (8, 9, 7, 10, 6, 11, 5, 12, 4, 13, 3, 14, 2, 15, 1, 0)
OUT_ORDER = [2 * chip + core for chip in CHIPS for core in (0, 1)]
BACK_CHIPS = (8, 9, 7, 10, 6, 11, 5, 12, 4, 13, 3, 14, 2, 15, 1, 0)
BACK_ORDER = [2 * chip + core for chip in BACK_CHIPS for core in (0, 1)]

f32 = jnp.float32
bf16 = jnp.bfloat16
VMEM = pl.BlockSpec(memory_space=pltpu.VMEM)
SMEM = pl.BlockSpec(memory_space=pltpu.SMEM)


def expert_of(slot, exp_here):
    piece = slot // (CAP * exp_here)
    place = piece // 2
    step = (place + 1) // 2
    chip = (CHIPS[0] + 16 + jnp.where(place % 2 == 1, step, -step)) % 16
    core = piece % 2
    return (chip * 2 + core) * exp_here + (slot // CAP) % exp_here


def iota(shape, dim):
    return lax.broadcasted_iota(jnp.int32, shape, dim)


def dot(a, b):
    return jnp.dot(a, b, preferred_element_type=f32)


def place_kernel(routing_ref, placing_ref):
    slots, rows = placing_ref.shape
    slot = iota((slots, rows), 0)
    expert = expert_of(slot, 2)
    chosen = jnp.zeros((slots, rows), f32)
    for k in range(routing_ref.shape[0]):
        chosen = jnp.where(routing_ref[k : k + 1, :] == expert, 1.0, chosen)
    before = (iota((rows, rows), 0) < iota((rows, rows), 1)).astype(f32).astype(bf16)
    rank = dot(chosen.astype(bf16), before).astype(jnp.int32)
    placing_ref[...] = jnp.where(rank == slot % CAP, chosen, 0.0).astype(bf16)


def place(routing, slots):
    return pl.pallas_call(
        place_kernel,
        out_shape=jax.ShapeDtypeStruct((slots, routing.shape[1]), bf16),
        in_specs=[VMEM],
        out_specs=VMEM,
        name="place",
        cost_estimate=pl.CostEstimate(flops=1 << 29, bytes_accessed=1 << 17, transcendentals=0),
        compiler_params=pltpu.CompilerParams(vmem_limit_bytes=8 << 20),
    )(routing)


def dispatch_kernel(placing_ref, tokens_ref, out_ref):
    placing = placing_ref[...]
    rows = dot(placing, tokens_ref[...])
    filled = dot(placing, jnp.ones(tokens_ref.shape, bf16))
    out_ref[...] = jnp.where(filled > 0.5, rows, EMPTY).astype(bf16)


def dispatch(placing, tokens):
    return pl.pallas_call(
        dispatch_kernel,
        out_shape=jax.ShapeDtypeStruct((placing.shape[0], tokens.shape[1]), bf16),
        in_specs=[VMEM] * 2,
        out_specs=VMEM,
        name="dispatch",
        compiler_params=pltpu.CompilerParams(vmem_limit_bytes=8 << 20),
    )(placing, tokens)


def order_key(index):
    return (index & CAP) * 512 + index


def order_kernel(received_ref, column_ref, row_ref, first_ref, bucket_ref):
    slots, width = received_ref.shape
    filled = received_ref[...].astype(f32) < FILLED_BELOW
    ones = jnp.where(filled, 1.0, 0.0).astype(bf16)
    own_key = order_key(iota((slots, width), 0))
    other_key = order_key(iota((1, slots), 1))
    later = [
        jnp.where(other_key[:, b : b + width] < own_key, 1.0, 0.0).astype(bf16)
        for b in range(0, slots, width)
    ]
    later = jnp.concatenate(later, axis=1)
    column = dot(later, ones)
    column_ref[...] = jnp.where(filled, column, -1.0)
    across = lax.dot_general(
        jnp.full((8, width), 1.0 / width, bf16),
        ones,
        (((1,), (1,)), ((), ())),
        preferred_element_type=f32,
    )
    total = jnp.sum(across[0:1, :], axis=1, keepdims=True)
    row = total - 1.0 - dot(across.astype(bf16), later)
    row_ref[...] = jnp.where(across > 0.5, row, -1.0)
    is_first = (iota((1, slots), 1) & CAP) == 0
    first = jnp.sum(jnp.where(is_first, across[0:1, :], 0.0), axis=1, keepdims=True)
    count = jnp.sum(across[0:1, :])
    bucket = jnp.int32(0)
    for size in BUCKETS[:-1]:
        bucket = bucket + (count > size).astype(jnp.int32)
    first_ref[...] = jnp.zeros(first_ref.shape, f32) + first
    bucket_ref[0] = bucket


def order_rows(received):
    slots, width = received.shape
    return pl.pallas_call(
        order_kernel,
        out_shape=(
            jax.ShapeDtypeStruct((slots, width), f32),
            jax.ShapeDtypeStruct((8, slots), f32),
            jax.ShapeDtypeStruct((8, width), f32),
            jax.ShapeDtypeStruct((1,), jnp.int32),
        ),
        in_specs=[VMEM],
        out_specs=(VMEM, VMEM, VMEM, SMEM),
        name="order_rows",
        compiler_params=pltpu.CompilerParams(vmem_limit_bytes=12 << 20),
    )(received)


def compact_kernel(received_ref, row_ref, gain_ref, out_ref):
    copies, size, _ = out_ref.shape
    slots = received_ref.shape[0]
    position = iota((size, slots), 0).astype(f32)
    pick = jnp.where(row_ref[0:1, :] == position, 1.0, 0.0).astype(bf16)
    gain = gain_ref[pl.ds(lax.axis_index(TP), 1), :]
    rows = (dot(pick, received_ref[...]) * gain).astype(bf16)
    for n in range(copies):
        out_ref[n] = rows


def compact(received, row, gain, size):
    copies = gain.shape[0]
    return pl.pallas_call(
        compact_kernel,
        out_shape=jax.ShapeDtypeStruct((copies, size, received.shape[1]), bf16),
        in_specs=[VMEM] * 3,
        out_specs=VMEM,
        name="compact",
        compiler_params=pltpu.CompilerParams(vmem_limit_bytes=12 << 20),
    )(received, row, gain)


def expert_kernel(first_ref, x_ref, gain_ref, gate_ref, up_ref, down_ref, out_ref):
    parts, size, width = x_ref.shape
    undo = 1.0 / (gain_ref[...] * gain_ref[...])
    ssq = jnp.zeros((size, width), f32)
    for p in range(parts):
        x = x_ref[p].astype(f32)
        q = TP_ORDER[p]
        ssq = ssq + x * x * undo[q : q + 1, :]
    scale = lax.rsqrt(jnp.sum(ssq, axis=1, keepdims=True) / D + norm_eps)
    rows = jnp.concatenate([x_ref[TP_ORDER.index(q)] for q in range(parts)], axis=1)
    row = iota((size, width), 0).astype(f32)
    first = first_ref[0:1, :]
    hidden = []
    for e in range(2):
        pre = dot(rows, jnp.concatenate([gate_ref[e], up_ref[e]], axis=1)) * scale
        clamped = jnp.minimum(pre[:, :width], clamp_limit)
        upper = jnp.clip(pre[:, width:], -clamp_limit, clamp_limit)
        value = clamped * jax.nn.sigmoid(swish_alpha * clamped) * (upper + 1.0)
        mine = row < first if e == 0 else row >= first
        hidden.append(jnp.where(mine, value, 0.0).astype(bf16))
    hidden = jnp.concatenate(hidden, axis=1)
    for p in range(0, parts, 2):
        out = dot(hidden, down_ref[:, p * width : (p + 2) * width]).astype(bf16)
        out_ref[TP_BACK_ORDER.index(p)] = out[:, :width]
        out_ref[TP_BACK_ORDER.index(p + 1)] = out[:, width:]


def experts(first, x, gain, gate, up, down):
    parts, size, width = x.shape
    return pl.pallas_call(
        expert_kernel,
        out_shape=jax.ShapeDtypeStruct(x.shape, bf16),
        in_specs=[VMEM] * 6,
        out_specs=VMEM,
        name="experts",
        compiler_params=pltpu.CompilerParams(vmem_limit_bytes=20 << 20),
    )(first, x, gain, gate, up, down)


def expand_kernel(parts_ref, column_ref, out_ref, total):
    parts, size, width = parts_ref.shape
    slots = column_ref.shape[0]
    padded = total.shape[0]
    value = parts_ref[0].astype(f32)
    for p in range(1, parts):
        value = value + parts_ref[p].astype(f32)
    if padded > size:
        total[...] = jnp.zeros(total.shape, bf16)
    total[:size, :] = value.astype(bf16)
    column = column_ref[...]
    lane = iota((slots, width), 1).astype(f32)
    picks = [
        jnp.where(column == lane + float(b * width), 1.0, 0.0).astype(bf16)
        for b in range(padded // width)
    ]
    out = dot(jnp.concatenate(picks, axis=1), total[...]).astype(bf16)
    piece = slots // len(OUT_ORDER)
    for n, member in enumerate(BACK_ORDER):
        at = OUT_ORDER.index(member) * piece
        out_ref[n * piece : (n + 1) * piece, :] = out[at : at + piece, :]


def expand(parts, column):
    _, size, width = parts.shape
    padded = -(-size // width) * width
    return pl.pallas_call(
        expand_kernel,
        out_shape=jax.ShapeDtypeStruct((column.shape[0], width), bf16),
        in_specs=[VMEM] * 2,
        out_specs=VMEM,
        scratch_shapes=[pltpu.VMEM((padded, width), bf16)],
        name="expand",
        compiler_params=pltpu.CompilerParams(vmem_limit_bytes=12 << 20),
    )(parts, column)


def combine_kernel(returned_ref, placing_ref, routing_ref, weight_ref, out_ref):
    slots, rows = placing_ref.shape
    expert = expert_of(iota((slots, rows), 0), 2)
    weight = jnp.zeros((slots, rows), f32)
    for k in range(routing_ref.shape[0]):
        weight = jnp.where(routing_ref[k : k + 1, :] == expert, weight_ref[k : k + 1, :], weight)
    weight = weight * placing_ref[...].astype(f32)
    high = weight.astype(bf16)
    low = (weight - high.astype(f32)).astype(bf16)
    contract = (((0,), (0,)), ((), ()))
    piece = slots // len(OUT_ORDER)
    places = [BACK_ORDER.index(member) * piece for member in OUT_ORDER]
    returned = jnp.concatenate([returned_ref[at : at + piece, :] for at in places], axis=0)
    mixed = lax.dot_general(high, returned, contract, preferred_element_type=f32)
    mixed = mixed + lax.dot_general(low, returned, contract, preferred_element_type=f32)
    out_ref[...] = mixed.astype(bf16)


def combine(returned, placing, routing, gate_weights):
    return pl.pallas_call(
        combine_kernel,
        out_shape=jax.ShapeDtypeStruct((placing.shape[1], returned.shape[1]), bf16),
        in_specs=[VMEM] * 4,
        out_specs=VMEM,
        name="combine",
        compiler_params=pltpu.CompilerParams(vmem_limit_bytes=8 << 20),
    )(returned, placing, routing, gate_weights)


def exchange(pieces, axis, order=None):
    groups = None if order is None else [order]
    return lax.all_to_all(
        pieces, axis, split_axis=0, concat_axis=0, axis_index_groups=groups, tiled=True
    )


def per_device(tokens, routing, gate_weights, norm_gain, w_gate, w_up, w_down):
    ep_size = lax.axis_size("ep")
    tp_size = lax.axis_size(TP)
    exp_here = w_gate.shape[0]
    width = tokens.shape[1]
    slots = ep_size * exp_here * CAP
    gain = norm_gain.reshape(tp_size, width)
    down = w_down.reshape(exp_here * w_down.shape[1], w_down.shape[2])
    placing = place(routing.T, slots)
    outgoing = dispatch(placing, tokens)
    received = exchange(outgoing.reshape(ep_size, exp_here * CAP, width), "ep", OUT_ORDER)
    received = received.reshape(slots, width)
    column, row, first, bucket = order_rows(received)

    def middle(size, received, column, row, first, gain, w_gate, w_up, down):
        rows = exchange(compact(received, row, gain, size), TP, TP_ORDER)
        partial_value = experts(first, rows, gain, w_gate, w_up, down)
        return expand(exchange(partial_value, TP, TP_BACK_ORDER), column)

    branches = [functools.partial(middle, size) for size in BUCKETS]
    operands = (received, column, row, first, gain, w_gate, w_up, down)
    if len(branches) == 1:
        back = branches[0](*operands)
    else:
        back = lax.switch(bucket[0], branches, *operands)
    returned = exchange(back.reshape(ep_size, exp_here * CAP, width), "ep", BACK_ORDER)
    return combine(returned.reshape(slots, width), placing, routing.T, gate_weights.T)


def solution(mesh):
    split = Mesh(mesh.devices.reshape(mesh.shape["ep"], 4, 4), ("ep", "tp_0", "tp_1"))
    placed = (
        P("ep", TP),
        P("ep", None),
        P("ep", None),
        P(),
        P("ep", None, TP),
        P("ep", None, TP),
        P("ep", TP, None),
    )
    return jax.shard_map(
        per_device, mesh=split, in_specs=placed, out_specs=P("ep", TP), check_vma=False
    )
```

```python
import functools

import jax
import jax.numpy as jnp
from jax import lax
from jax.experimental import pallas as pl
from jax.experimental.pallas import tpu as pltpu
from jax.sharding import Mesh
from jax.sharding import PartitionSpec as P

D = 2048
CAP = 8
TP = ("tp_0", "tp_1")
BUCKETS = (144, 176, 208, 240, 272, 304, 336, 368, 432, 512)

norm_eps = 1e-06
clamp_limit = 7.0
swish_alpha = 1.702
EMPTY = 512.0
FILLED_BELOW = 256.0

TP_ORDER = [10, 11, 8, 9, 13, 14, 15, 12, 0, 1, 2, 3, 7, 4, 5, 6]
TP_BACK_ORDER = [10, 11, 8, 9, 13, 14, 15, 12, 0, 1, 2, 3, 7, 4, 5, 6]

CHIPS = (8, 9, 7, 10, 6, 11, 5, 12, 4, 13, 3, 14, 2, 15, 1, 0)
OUT_ORDER = [2 * chip + core for chip in CHIPS for core in (1, 0)]
BACK_CHIPS = (8, 9, 7, 10, 6, 11, 5, 12, 4, 13, 3, 14, 2, 15, 1, 0)
BACK_ORDER = [2 * chip + core for chip in BACK_CHIPS for core in (1, 0)]

f32 = jnp.float32
bf16 = jnp.bfloat16
VMEM = pl.BlockSpec(memory_space=pltpu.VMEM)
SMEM = pl.BlockSpec(memory_space=pltpu.SMEM)


def expert_of(slot, exp_here):
    piece = slot // (CAP * exp_here)
    place = piece // 2
    step = (place + 1) // 2
    chip = (CHIPS[0] + 16 + jnp.where(place % 2 == 1, step, -step)) % 16
    core = 1 - piece % 2
    return (chip * 2 + core) * exp_here + (slot // CAP) % exp_here


def iota(shape, dim):
    return lax.broadcasted_iota(jnp.int32, shape, dim)


def dot(a, b):
    return jnp.dot(a, b, preferred_element_type=f32)


def place_kernel(routing_ref, placing_ref):
    slots, rows = placing_ref.shape
    slot = iota((slots, rows), 0)
    expert = expert_of(slot, 2)
    chosen = jnp.zeros((slots, rows), f32)
    for k in range(routing_ref.shape[0]):
        chosen = jnp.where(routing_ref[k : k + 1, :] == expert, 1.0, chosen)
    before = (iota((rows, rows), 0) < iota((rows, rows), 1)).astype(f32).astype(bf16)
    rank = dot(chosen.astype(bf16), before).astype(jnp.int32)
    placing_ref[...] = jnp.where(rank == slot % CAP, chosen, 0.0).astype(bf16)


def place(routing, slots):
    return pl.pallas_call(
        place_kernel,
        out_shape=jax.ShapeDtypeStruct((slots, routing.shape[1]), bf16),
        in_specs=[VMEM],
        out_specs=VMEM,
        name="place",
        cost_estimate=pl.CostEstimate(flops=1 << 29, bytes_accessed=1 << 17, transcendentals=0),
        compiler_params=pltpu.CompilerParams(vmem_limit_bytes=8 << 20),
    )(routing)


def dispatch_kernel(placing_ref, tokens_ref, out_ref):
    placing = placing_ref[...]
    rows = dot(placing, tokens_ref[...])
    filled = dot(placing, jnp.ones(tokens_ref.shape, bf16))
    out_ref[...] = jnp.where(filled > 0.5, rows, EMPTY).astype(bf16)


def dispatch(placing, tokens):
    return pl.pallas_call(
        dispatch_kernel,
        out_shape=jax.ShapeDtypeStruct((placing.shape[0], tokens.shape[1]), bf16),
        in_specs=[VMEM] * 2,
        out_specs=VMEM,
        name="dispatch",
        compiler_params=pltpu.CompilerParams(vmem_limit_bytes=8 << 20),
    )(placing, tokens)


def order_key(index):
    return (index & CAP) * 512 + index


def order_kernel(received_ref, column_ref, row_ref, first_ref, bucket_ref):
    slots, width = received_ref.shape
    filled = received_ref[...].astype(f32) < FILLED_BELOW
    ones = jnp.where(filled, 1.0, 0.0).astype(bf16)
    own_key = order_key(iota((slots, width), 0))
    other_key = order_key(iota((1, slots), 1))
    later = [
        jnp.where(other_key[:, b : b + width] < own_key, 1.0, 0.0).astype(bf16)
        for b in range(0, slots, width)
    ]
    later = jnp.concatenate(later, axis=1)
    column = dot(later, ones)
    column_ref[...] = jnp.where(filled, column, -1.0)
    across = lax.dot_general(
        jnp.full((8, width), 1.0 / width, bf16),
        ones,
        (((1,), (1,)), ((), ())),
        preferred_element_type=f32,
    )
    total = jnp.sum(across[0:1, :], axis=1, keepdims=True)
    row = total - 1.0 - dot(across.astype(bf16), later)
    row_ref[...] = jnp.where(across > 0.5, row, -1.0)
    is_first = (iota((1, slots), 1) & CAP) == 0
    first = jnp.sum(jnp.where(is_first, across[0:1, :], 0.0), axis=1, keepdims=True)
    count = jnp.sum(across[0:1, :])
    bucket = jnp.int32(0)
    for size in BUCKETS[:-1]:
        bucket = bucket + (count > size).astype(jnp.int32)
    first_ref[...] = jnp.zeros(first_ref.shape, f32) + first
    bucket_ref[0] = bucket


def order_rows(received):
    slots, width = received.shape
    return pl.pallas_call(
        order_kernel,
        out_shape=(
            jax.ShapeDtypeStruct((slots, width), f32),
            jax.ShapeDtypeStruct((8, slots), f32),
            jax.ShapeDtypeStruct((8, width), f32),
            jax.ShapeDtypeStruct((1,), jnp.int32),
        ),
        in_specs=[VMEM],
        out_specs=(VMEM, VMEM, VMEM, SMEM),
        name="order_rows",
        compiler_params=pltpu.CompilerParams(vmem_limit_bytes=12 << 20),
    )(received)


def compact_kernel(received_ref, row_ref, gain_ref, out_ref):
    copies, size, _ = out_ref.shape
    slots = received_ref.shape[0]
    position = iota((size, slots), 0).astype(f32)
    pick = jnp.where(row_ref[0:1, :] == position, 1.0, 0.0).astype(bf16)
    gain = gain_ref[pl.ds(lax.axis_index(TP), 1), :]
    rows = (dot(pick, received_ref[...]) * gain).astype(bf16)
    for n in range(copies):
        out_ref[n] = rows


def compact(received, row, gain, size):
    copies = gain.shape[0]
    return pl.pallas_call(
        compact_kernel,
        out_shape=jax.ShapeDtypeStruct((copies, size, received.shape[1]), bf16),
        in_specs=[VMEM] * 3,
        out_specs=VMEM,
        name="compact",
        compiler_params=pltpu.CompilerParams(vmem_limit_bytes=12 << 20),
    )(received, row, gain)


def expert_kernel(first_ref, x_ref, gain_ref, gate_ref, up_ref, down_ref, out_ref):
    parts, size, width = x_ref.shape
    undo = 1.0 / (gain_ref[...] * gain_ref[...])
    ssq = jnp.zeros((size, width), f32)
    for p in range(parts):
        x = x_ref[p].astype(f32)
        q = TP_ORDER[p]
        ssq = ssq + x * x * undo[q : q + 1, :]
    scale = lax.rsqrt(jnp.sum(ssq, axis=1, keepdims=True) / D + norm_eps)
    rows = jnp.concatenate([x_ref[TP_ORDER.index(q)] for q in range(parts)], axis=1)
    row = iota((size, width), 0).astype(f32)
    first = first_ref[0:1, :]
    hidden = []
    for e in range(2):
        pre = dot(rows, jnp.concatenate([gate_ref[e], up_ref[e]], axis=1)) * scale
        clamped = jnp.minimum(pre[:, :width], clamp_limit)
        upper = jnp.clip(pre[:, width:], -clamp_limit, clamp_limit)
        value = clamped * jax.nn.sigmoid(swish_alpha * clamped) * (upper + 1.0)
        mine = row < first if e == 0 else row >= first
        hidden.append(jnp.where(mine, value, 0.0).astype(bf16))
    hidden = jnp.concatenate(hidden, axis=1)
    for p in range(0, parts, 2):
        out = dot(hidden, down_ref[:, p * width : (p + 2) * width]).astype(bf16)
        out_ref[TP_BACK_ORDER.index(p)] = out[:, :width]
        out_ref[TP_BACK_ORDER.index(p + 1)] = out[:, width:]


def experts(first, x, gain, gate, up, down):
    parts, size, width = x.shape
    return pl.pallas_call(
        expert_kernel,
        out_shape=jax.ShapeDtypeStruct(x.shape, bf16),
        in_specs=[VMEM] * 6,
        out_specs=VMEM,
        name="experts",
        compiler_params=pltpu.CompilerParams(vmem_limit_bytes=20 << 20),
    )(first, x, gain, gate, up, down)


def expand_kernel(parts_ref, column_ref, out_ref, total):
    parts, size, width = parts_ref.shape
    slots = column_ref.shape[0]
    padded = total.shape[0]
    value = parts_ref[0].astype(f32)
    for p in range(1, parts):
        value = value + parts_ref[p].astype(f32)
    if padded > size:
        total[...] = jnp.zeros(total.shape, bf16)
    total[:size, :] = value.astype(bf16)
    column = column_ref[...]
    lane = iota((slots, width), 1).astype(f32)
    picks = [
        jnp.where(column == lane + float(b * width), 1.0, 0.0).astype(bf16)
        for b in range(padded // width)
    ]
    out = dot(jnp.concatenate(picks, axis=1), total[...]).astype(bf16)
    piece = slots // len(OUT_ORDER)
    for n, member in enumerate(BACK_ORDER):
        at = OUT_ORDER.index(member) * piece
        out_ref[n * piece : (n + 1) * piece, :] = out[at : at + piece, :]


def expand(parts, column):
    _, size, width = parts.shape
    padded = -(-size // width) * width
    return pl.pallas_call(
        expand_kernel,
        out_shape=jax.ShapeDtypeStruct((column.shape[0], width), bf16),
        in_specs=[VMEM] * 2,
        out_specs=VMEM,
        scratch_shapes=[pltpu.VMEM((padded, width), bf16)],
        name="expand",
        compiler_params=pltpu.CompilerParams(vmem_limit_bytes=12 << 20),
    )(parts, column)


def combine_kernel(returned_ref, placing_ref, routing_ref, weight_ref, out_ref):
    slots, rows = placing_ref.shape
    expert = expert_of(iota((slots, rows), 0), 2)
    weight = jnp.zeros((slots, rows), f32)
    for k in range(routing_ref.shape[0]):
        weight = jnp.where(routing_ref[k : k + 1, :] == expert, weight_ref[k : k + 1, :], weight)
    weight = weight * placing_ref[...].astype(f32)
    high = weight.astype(bf16)
    low = (weight - high.astype(f32)).astype(bf16)
    contract = (((0,), (0,)), ((), ()))
    piece = slots // len(OUT_ORDER)
    places = [BACK_ORDER.index(member) * piece for member in OUT_ORDER]
    returned = jnp.concatenate([returned_ref[at : at + piece, :] for at in places], axis=0)
    mixed = lax.dot_general(high, returned, contract, preferred_element_type=f32)
    mixed = mixed + lax.dot_general(low, returned, contract, preferred_element_type=f32)
    out_ref[...] = mixed.astype(bf16)


def combine(returned, placing, routing, gate_weights):
    return pl.pallas_call(
        combine_kernel,
        out_shape=jax.ShapeDtypeStruct((placing.shape[1], returned.shape[1]), bf16),
        in_specs=[VMEM] * 4,
        out_specs=VMEM,
        name="combine",
        compiler_params=pltpu.CompilerParams(vmem_limit_bytes=8 << 20),
    )(returned, placing, routing, gate_weights)


def exchange(pieces, axis, order=None):
    groups = None if order is None else [order]
    return lax.all_to_all(
        pieces, axis, split_axis=0, concat_axis=0, axis_index_groups=groups, tiled=True
    )


def per_device(tokens, routing, gate_weights, norm_gain, w_gate, w_up, w_down):
    ep_size = lax.axis_size("ep")
    tp_size = lax.axis_size(TP)
    exp_here = w_gate.shape[0]
    width = tokens.shape[1]
    slots = ep_size * exp_here * CAP
    gain = norm_gain.reshape(tp_size, width)
    down = w_down.reshape(exp_here * w_down.shape[1], w_down.shape[2])
    placing = place(routing.T, slots)
    outgoing = dispatch(placing, tokens)
    received = exchange(outgoing.reshape(ep_size, exp_here * CAP, width), "ep", OUT_ORDER)
    received = received.reshape(slots, width)
    column, row, first, bucket = order_rows(received)

    def middle(size, received, column, row, first, gain, w_gate, w_up, down):
        rows = exchange(compact(received, row, gain, size), TP, TP_ORDER)
        partial_value = experts(first, rows, gain, w_gate, w_up, down)
        return expand(exchange(partial_value, TP, TP_BACK_ORDER), column)

    branches = [functools.partial(middle, size) for size in BUCKETS]
    operands = (received, column, row, first, gain, w_gate, w_up, down)
    if len(branches) == 1:
        back = branches[0](*operands)
    else:
        back = lax.switch(bucket[0], branches, *operands)
    returned = exchange(back.reshape(ep_size, exp_here * CAP, width), "ep", BACK_ORDER)
    return combine(returned.reshape(slots, width), placing, routing.T, gate_weights.T)


def solution(mesh):
    split = Mesh(mesh.devices.reshape(mesh.shape["ep"], 4, 4), ("ep", "tp_0", "tp_1"))
    placed = (
        P("ep", TP),
        P("ep", None),
        P("ep", None),
        P(),
        P("ep", None, TP),
        P("ep", None, TP),
        P("ep", TP, None),
    )
    return jax.shard_map(
        per_device, mesh=split, in_specs=placed, out_specs=P("ep", TP), check_vma=False
    )
```
